32 devices in a mesh: ep: 32 (over z, y, x, core).
Axes of the slice: x: 2, y: 2, z: 4, core: 2. Of those that a mesh axis runs over, the one named last changes fastest.
Arguments:
- tokens: bfloat16 [8192, 2048], P('ep'), may hold values from -6 to 6
- norm_gain: float32 [2048], replicated, may hold values from 0.1 to 1.9
- expert_ids: int32 [8192, 2], P('ep'), may hold values from 0 to 31, as said below
- gates: float32 [8192, 2], P('ep'), may hold values from 0.1 to 1
- w_gate: bfloat16 [32, 2048, 1024], P('ep'), may hold values from -0.125 to 0.125
- w_up: bfloat16 [32, 2048, 1024], P('ep'), may hold values from -0.125 to 0.125
- w_down: bfloat16 [32, 1024, 2048], P('ep'), may hold values from -0.1875 to 0.1875
Outputs:
- combined: bfloat16 [8192, 2048], P('ep')
The draws below stay inside these ranges and needn't reach their ends.
Inputs may be any that keep to these rules, and one draw needn't show every extreme that they name: `expert_ids`: each row names two different experts of one group, a group being 4 consecutive expert numbers. Among the rows of one device no expert is named more than 32 times, and some expert is named exactly 32 times; some expert is named exactly 32 times by the rows of every device.
All inputs are finite; a program needn't handle non-finite values.
Results may differ from the reference program's by a relative error of at most 0.0085.
Values may be sent and summed in bfloat16 or wider, within the bound.
A program may use at most 128 MiB of HBM per device.

```python
import jax
import jax.numpy as jnp
from jax import lax

D = 2048
FF = 1024
GROUP_EXPERTS = 4
TOK_DEV = 256
EXPERTS = 32
CAP = 32
TOKENS = 8192
N_EP = 32


def draw_expert_ids(key, part):
    groups = EXPERTS // GROUP_EXPERTS
    pool_size = groups * 2 * CAP
    popularity = jax.random.randint(jax.random.fold_in(key, 11), (groups,), 0, 4)
    common = jax.random.randint(jax.random.fold_in(key, 13), (), 0, groups)
    slot_group = jnp.arange(pool_size, dtype=jnp.int32) // (2 * CAP)
    slot_position = jnp.arange(pool_size, dtype=jnp.int32) % (2 * CAP)

    def one_block(block_index):
        subkeys = jax.random.split(jax.random.fold_in(jax.random.fold_in(key, 17), block_index), 5)
        chosen_group = jax.random.randint(subkeys[0], (), 0, groups)
        jitter = jax.random.randint(subkeys[1], (pool_size,), 0, 4096)
        priority = popularity[slot_group] * 2048 + jitter
        priority = jnp.where(slot_group == chosen_group, 16384 + jitter, priority)
        priority = jnp.where(slot_group == common, 32768 + jitter, priority)
        priority = priority * pool_size + jnp.arange(pool_size, dtype=jnp.int32)
        _, picked = lax.top_k(priority, TOK_DEV)
        picked = picked[jax.random.permutation(subkeys[2], TOK_DEV)]
        group_of = slot_group[picked]
        position = slot_position[picked]
        ranks = jax.random.randint(subkeys[3], (groups, GROUP_EXPERTS), 0, 1 << 20) * GROUP_EXPERTS
        orders = jnp.argsort(ranks + jnp.arange(GROUP_EXPERTS, dtype=jnp.int32)[None, :], axis=1)
        rotation = jax.random.randint(subkeys[4], (groups,), 0, 3)
        quarter = position % 4
        offset = 1 + (position // 4 + rotation[group_of]) % 3
        first_local = orders[group_of, quarter]
        second = orders[group_of, (quarter + offset) % 4]
        return jnp.stack([group_of * GROUP_EXPERTS + first_local, group_of * GROUP_EXPERTS + second], axis=1).astype(jnp.int32)
    drawn = jax.vmap(one_block)(jnp.arange(TOKENS // TOK_DEV, dtype=jnp.int32))
    return drawn.reshape(TOKENS, 2).astype(jnp.int32)


def levels(own_key, shape, shards, low, top_value):
    def one(dim, shards_of):
        steps = jax.random.uniform(jax.random.fold_in(jax.random.fold_in(own_key, 6), dim), (shards_of,), jnp.float32, low / len(shards), top_value / len(shards))
        return jnp.repeat(jnp.exp(steps), shape[dim] // shards_of).reshape((-1,) + (1,) * (len(shape) - dim - 1))

    level = one(*shards[0])
    for cut in shards[1:]:
        level = level * one(*cut)
    return level


def scatter_about(rng, dims, deviation, reach, pieces=(), kind=jnp.bfloat16):
    values = jax.random.normal(rng, dims, jnp.float32) * deviation
    if len(pieces) > 0:
        values = levels(rng, dims, pieces, -0.22, 0.18) * values
    return jnp.clip(values, min=-reach, max=reach).astype(kind)


def setup_inputs(seed: int = 0) -> dict:
    splits = jax.random.split(jax.random.key(seed), 8)
    return {
        "tokens": scatter_about(splits[0], (TOKENS, D), 1.0, 6.0, ((0, 32),)),
        "norm_gain": jnp.clip(1.0 + 0.18 * jax.random.normal(splits[1], (D,), jnp.float32), 0.1, 1.9),
        "expert_ids": draw_expert_ids(jax.random.fold_in(splits[7], 71), 0),
        "gates": jnp.clip(0.1 + 0.9 * jax.random.uniform(splits[3], (TOKENS, 2), jnp.float32) ** levels(splits[3], (TOKENS, 2), ((0, 32),), -0.2, 0.2), 0.1, 1.0),
        "w_gate": scatter_about(splits[4], (EXPERTS, D, FF), D ** -0.5, 0.125, ((0, 32),)),
        "w_up": scatter_about(splits[5], (EXPERTS, D, FF), D ** -0.5, 0.125, ((0, 32),)),
        "w_down": scatter_about(splits[6], (EXPERTS, FF, D), FF ** -0.5, 0.1875, ((0, 32),)),
    }


EPS = 1e-06

def normalize(tokens, norm_gain):
    floats = tokens.astype(jnp.float32)
    inverse_rms = lax.rsqrt(lax.optimization_barrier(jnp.mean(floats * floats, axis=-1, keepdims=True)) + EPS)
    return (floats * inverse_rms * norm_gain.astype(jnp.float32)).astype(jnp.bfloat16)

def expert_rows(block_rows, gate_weight, up_weight, down_weight):
    gate_part = jnp.dot(block_rows, gate_weight, preferred_element_type=jnp.float32)
    up_part = jnp.dot(block_rows, up_weight, preferred_element_type=jnp.float32)
    hidden = (jax.nn.silu(gate_part) * up_part).astype(jnp.bfloat16)
    return jnp.dot(hidden, down_weight, preferred_element_type=jnp.float32).astype(jnp.bfloat16)

def reference(tokens, norm_gain, expert_ids, gates, w_gate, w_up, w_down):
    normed = normalize(tokens, norm_gain)
    blocks = N_EP
    grouped_ids = expert_ids.astype(jnp.int32).reshape(blocks, 2 * TOK_DEV)
    one_hot = (grouped_ids[:, :, None] == jnp.arange(EXPERTS, dtype=jnp.int32)[None, None, :]).astype(jnp.int32)
    earlier = jnp.cumsum(one_hot, axis=1) - one_hot
    slot_index = lax.optimization_barrier(jnp.sum(earlier * one_hot, axis=2)).astype(jnp.int32)
    block_index = jnp.arange(blocks, dtype=jnp.int32)[:, None]
    buffer_row = ((grouped_ids * blocks + block_index) * CAP + slot_index).reshape(-1).astype(jnp.int32)
    token_row = (jnp.arange(2 * TOKENS, dtype=jnp.int32) // 2).astype(jnp.int32)
    source_row = jnp.full((EXPERTS * blocks * CAP,), TOKENS, jnp.int32).at[buffer_row].set(token_row)
    source_row = source_row.reshape(EXPERTS, blocks * CAP)
    weight_row = jnp.zeros((EXPERTS * blocks * CAP,), jnp.float32).at[buffer_row].set(gates.reshape(-1).astype(jnp.float32))
    weight_row = weight_row.reshape(EXPERTS, blocks * CAP)
    padded = jnp.concatenate([normed, jnp.zeros((1, D), jnp.bfloat16)], axis=0)

    def add_expert(accumulated, inputs):
        rows_index, row_weight, gate_weight, up_weight, down_weight = inputs
        block_rows = jnp.take(padded, rows_index, axis=0)
        produced = expert_rows(block_rows, gate_weight, up_weight, down_weight)
        update = row_weight[:, None] * produced.astype(jnp.float32)
        return (accumulated.at[rows_index].add(update), None)
    initial = jnp.zeros((TOKENS + 1, D), jnp.float32)
    accumulated, _ = lax.scan(add_expert, initial, (source_row, weight_row, w_gate, w_up, w_down))
    return accumulated[:TOKENS].astype(jnp.bfloat16)
```

```python
import functools

import jax
import jax.numpy as jnp
from jax import lax
from jax.experimental import pallas as pl
from jax.experimental.pallas import tpu as pltpu
from jax.sharding import PartitionSpec as P

EPS = 1e-06
MEMBERS = 4
LANES = 128
MESH = pl.DeviceIdType.MESH
F32 = jnp.float32
BF16 = jnp.bfloat16


def xor(a, b, count):
    total, bit = 0, 1
    while bit < count:
        total = total + ((a // bit + b // bit) % 2) * bit
        bit *= 2
    return total


def bits(i):
    return bin(i).count("1")


def select_order(groups):
    half = groups // 2
    upper = sorted(range(half, groups), key=lambda i: (bits(i), -i))
    lower = sorted(range(1, half), key=lambda i: (bits(i), i))
    order, lower = [0, *lower[:2]], lower[2:]
    while upper or lower:
        order += upper[:2] + lower[:1]
        upper, lower = upper[2:], lower[1:]
    return order


def output_order(groups):
    order = select_order(groups)
    half = groups // 2
    return [i for i in order if i >= half] + [i for i in order if 0 < i < half] + [0]


def output_lag(groups):
    first, second = select_order(groups), output_order(groups)
    return 1 + max(first.index(i) - second.index(i) for i in range(groups))


def send_order(groups, distance):
    return [i for i in select_order(groups) if bits(i) == distance]


def entry(table, t):
    return sum(jnp.where(t == k, value, 0) for k, value in enumerate(table))


def merge_rows(block):
    parts, rows, width = block.shape
    if rows % 16 == 0:
        return block.reshape(parts * rows, width)
    return block.astype(F32).reshape(parts * rows, width).astype(BF16)


def split_rows(block, parts):
    rows, width = block.shape
    return block.reshape(parts, rows // parts, width).astype(BF16)


def chunks(width, size):
    size = min(width, size)
    return [slice(start, start + size) for start in range(0, width, size)]


def dot(a, b):
    return jnp.dot(a, b, preferred_element_type=F32)


def kernel(
    groups, cap,
    ids_hbm, gates_hbm, tokens_hbm, gain_hbm, wg_hbm, wu_hbm, wd_hbm, out_ref,
    ids_ref, gates_ref, tokens_ref, gain_ref, wg, wu, wd, normed, pack, pack_meta, blk, meta, sel, rows, hidden, outs, obuf, comb, back,
    in_sem, w_sem, near_sem, s1_send, s1_recv, m_send, m_recv, s2_send, s2_recv, r2_send, r2_recv, r1_send, r1_recv,
):
    tok, width = tokens_ref.shape
    ff = wg.shape[1]
    slots = 2 * cap
    experts = groups * MEMBERS
    me = lax.axis_index("ep")
    group, member = me // MEMBERS, me % MEMBERS

    def far(i):
        return xor(group, i, groups) * MEMBERS + member

    def near(k):
        return group * MEMBERS + xor(member, k, MEMBERS)

    distances = bits(groups - 1)
    barrier = pltpu.get_barrier_semaphore()
    for k in range(1, MEMBERS):
        pl.semaphore_signal(barrier, inc=1, device_id=(near(k),), device_id_type=MESH)
    for b in range(distances):
        pl.semaphore_signal(barrier, inc=1, device_id=(far(2**b),), device_id_type=MESH)

    block = min(tok, 64)
    small = [
        pltpu.make_async_copy(src, dst, in_sem.at[k])
        for k, (src, dst) in enumerate(((ids_hbm, ids_ref), (gates_hbm, gates_ref), (gain_hbm, gain_ref)))
    ]
    token_loads = [
        pltpu.make_async_copy(
            tokens_hbm.at[pl.ds(r, block)], tokens_ref.at[pl.ds(r, block)], in_sem.at[3 + r // block]
        )
        for r in range(0, tok, block)
    ]
    loads = [
        pltpu.make_async_copy(src.at[0], dst, w_sem.at[k])
        for k, (src, dst) in enumerate(((wg_hbm, wg), (wu_hbm, wu), (wd_hbm, wd)))
    ]
    for load in small + token_loads + loads:
        load.start()
    for load in small:
        load.wait()

    ids = ids_ref[...]
    first, second = ids[0:1, :], ids[1:2, :]
    before = (
        lax.broadcasted_iota(jnp.int32, (tok, tok), 0) < lax.broadcasted_iota(jnp.int32, (tok, tok), 1)
    ).astype(F32).astype(BF16)
    expert_iota = lax.broadcasted_iota(jnp.int32, (experts, tok), 0)
    is_first = (expert_iota == first).astype(F32)
    is_second = (expert_iota == second).astype(F32)
    earlier = dot((is_first + is_second).astype(BF16), before)
    place_first = jnp.sum(earlier * is_first, axis=0, keepdims=True) + 1.0
    place_second = jnp.sum(earlier * is_second, axis=0, keepdims=True) + 1.0
    token_group = first // MEMBERS
    group_rows = max(groups, 8)
    is_group = (lax.broadcasted_iota(jnp.int32, (group_rows, tok), 0) == token_group).astype(F32)
    slot = jnp.sum(dot(is_group.astype(BF16), before) * is_group, axis=0, keepdims=True).astype(jnp.int32)
    step_of = xor(token_group, jnp.full_like(token_group, group), groups)
    key = step_of * slots + slot

    local_first, local_second = first % MEMBERS, second % MEMBERS
    gates = gates_ref[...]
    gate_high = gates.astype(BF16).astype(F32)
    gate_low = (gates - gate_high).astype(BF16).astype(F32)

    def member_rows(of_first, of_second):
        m = lax.broadcasted_iota(jnp.int32, (8, tok), 0)
        return jnp.where(m == local_first, of_first, 0.0) + jnp.where(m == local_second, of_second, 0.0)

    facts = jnp.concatenate(
        [
            member_rows(place_first, place_second),
            member_rows(gate_high[0:1, :], gate_high[1:2, :]),
            member_rows(gate_low[0:1, :], gate_low[1:2, :]),
            jnp.zeros((8, tok), F32),
        ],
        axis=0,
    ).astype(BF16)
    pick_iota = lax.broadcasted_iota(jnp.int32, (groups * slots, tok), 0)
    picked = (pick_iota == key).astype(F32).astype(BF16)
    wide_iota = lax.broadcasted_iota(jnp.int32, (groups * LANES, tok), 0)
    wide = (wide_iota == step_of * LANES + slot).astype(F32).astype(BF16)
    told = lax.dot_general(
        facts, wide, (((1,), (1,)), ((), ())), preferred_element_type=F32
    ).astype(BF16)
    meta[0] = told[:, :LANES]
    for i in range(1, groups):
        pack_meta[i] = told[:, i * LANES : (i + 1) * LANES]
    for r in range(0, tok, block):
        token_loads[r // block].wait()
        part = pl.ds(r, block)
        floats = tokens_ref[part, :].astype(F32)
        inverse = lax.rsqrt(jnp.mean(floats * floats, axis=-1, keepdims=True) + EPS)
        normed[part, :] = (floats * inverse * gain_ref[...]).astype(BF16)

    for cols in chunks(width, 256):
        packed = split_rows(dot(picked, normed[:, cols]), groups)
        blk[0, :, cols] = packed[0]
        pack[1:, :, cols] = packed[1:]

    def s1_copy(i):
        return pltpu.make_async_remote_copy(
            src_ref=pack.at[i], dst_ref=blk.at[i], send_sem=s1_send.at[i], recv_sem=s1_recv.at[i],
            device_id=(far(i),), device_id_type=MESH,
        )

    def meta_copy(i):
        return pltpu.make_async_remote_copy(
            src_ref=pack_meta.at[i], dst_ref=meta.at[i], send_sem=m_send.at[i], recv_sem=m_recv.at[i],
            device_id=(far(i),), device_id_type=MESH,
        )

    def s2_copy(i, k):
        peer = xor(member, k, MEMBERS)
        return pltpu.make_async_remote_copy(
            src_ref=sel.at[i, peer], dst_ref=rows.at[i, member],
            send_sem=s2_send.at[i, k], recv_sem=s2_recv.at[i, k],
            device_id=(near(k),), device_id_type=MESH,
        )

    def r2_copy(i, k):
        peer = xor(member, k, MEMBERS)
        return pltpu.make_async_remote_copy(
            src_ref=outs.at[i, peer], dst_ref=obuf.at[i, member],
            send_sem=r2_send.at[i, k], recv_sem=r2_recv.at[i, k],
            device_id=(near(k),), device_id_type=MESH,
        )

    def r1_copy(i):
        return pltpu.make_async_remote_copy(
            src_ref=comb.at[i], dst_ref=back.at[i], send_sem=r1_send.at[i], recv_sem=r1_recv.at[i],
            device_id=(far(i),), device_id_type=MESH,
        )

    def send(distance):
        if distance == 1:
            pl.semaphore_wait(barrier, MEMBERS - 1 + distances)
        else:
            pl.semaphore_wait(near_sem.at[distance], distances)
        if distance < distances:
            for b in range(distances):
                pl.semaphore_signal(
                    near_sem.at[distance + 1], inc=1, device_id=(far(2**b),), device_id_type=MESH
                )
        for i in send_order(groups, distance):
            meta_copy(i).start()
            s1_copy(i).start()

    send(1)

    place_iota = lax.broadcasted_iota(jnp.int32, (cap, LANES), 0).astype(F32) + 1.0

    def one_hots(i):
        info = meta[i].astype(F32)
        return info, [(place_iota == info[m : m + 1, :]) for m in range(MEMBERS)]

    def select(i):
        @pl.when(i > 0)
        def _():
            meta_copy(i).wait_recv()
            s1_copy(i).wait_recv()

        _, hots = one_hots(i)
        pick = jnp.concatenate([h.astype(F32) for h in hots], axis=0).astype(BF16)[:, :slots]
        for cols in chunks(width, 512):
            sel[i, :, :, cols] = split_rows(dot(pick, blk[i, :, cols]), MEMBERS)
        for k in (2, 3, 1):
            s2_copy(i, k).start()
        rows[i, member] = sel[i, member]

    def ffn(i, is_first):
        @pl.when(is_first)
        def _():
            for load in loads:
                load.wait()

        for k in range(1, MEMBERS):
            s2_copy(i, k).wait_recv()
        x = merge_rows(rows[i])
        for cols in chunks(ff, 256):
            gate_part = dot(x, wg[:, cols])
            up_part = dot(x, wu[:, cols])
            hidden[:, cols] = (gate_part / (1.0 + jnp.exp(-gate_part)) * up_part).astype(BF16)
        h = hidden[...]
        for cols in chunks(width, 256):
            outs[i, :, :, cols] = split_rows(dot(h, wd[:, cols]), MEMBERS)
        for k in (2, 3, 1):
            r2_copy(i, k).start()
        obuf[i, member] = outs[i, member]

    def mix(i):
        for k in range(1, MEMBERS):
            r2_copy(i, k).wait_recv()
        info, hots = one_hots(i)

        def weights(row):
            parts = [jnp.where(hots[m], info[row + m : row + m + 1, :], 0.0) for m in range(MEMBERS)]
            return jnp.concatenate(parts, axis=0).T[:slots].astype(BF16)

        high, low = weights(8), weights(16)

        def mixed(cols):
            values = merge_rows(obuf[i, :, :, cols])
            return (dot(high, values) + dot(low, values)).astype(BF16)

        @pl.when(i == 0)
        def _():
            for cols in chunks(width, 512):
                back[0, :, cols] = mixed(cols)

        @pl.when(i > 0)
        def _():
            for cols in chunks(width, 512):
                comb[i, :, cols] = mixed(cols)
            r1_copy(i).start()

    first, second, lag = select_order(groups), output_order(groups), output_lag(groups)

    @pl.loop(0, groups + lag + 1)
    def _(t):
        @pl.when(t < groups)
        def _():
            select(entry(first, t))

        for d in range(2, distances + 1):
            @pl.when(t == d - 2)
            def _():
                send(d)

        @pl.when((t >= lag) & (t < groups + lag))
        def _():
            ffn(entry(second, t - lag), t == lag)

        @pl.when(t >= lag + 1)
        def _():
            mix(entry(second, t - lag - 1))

    key_column = jnp.broadcast_to(key.astype(F32), (LANES, tok)).T[:, 0:1].astype(jnp.int32)
    spread = (
        lax.broadcasted_iota(jnp.int32, (tok, groups * slots), 1) == key_column
    ).astype(F32).astype(BF16)

    @pl.loop(1, groups)
    def _(i):
        r1_copy(i).wait_recv()

    for cols in chunks(width, 256):
        out_ref[:, cols] = dot(spread, merge_rows(back[:, :, cols])).astype(BF16)

    @pl.loop(0, groups)
    def _(i):
        @pl.when(i > 0)
        def _():
            meta_copy(i).wait_send()
            s1_copy(i).wait_send()
            r1_copy(i).wait_send()

        for k in range(1, MEMBERS):
            s2_copy(i, k).wait_send()
            r2_copy(i, k).wait_send()


def shards(tokens, norm_gain, expert_ids, gates, w_gate, w_up, w_down):
    tok, width = tokens.shape
    ff = w_gate.shape[2]
    experts = lax.axis_size("ep")
    groups = experts // MEMBERS
    cap = 2 * ((2 * tok + experts - 1) // experts)
    slots = 2 * cap
    vmem = pl.BlockSpec(memory_space=pltpu.VMEM)
    hbm = pl.BlockSpec(memory_space=pl.ANY)
    dma = pltpu.SemaphoreType.DMA
    by_group = pltpu.VMEM((groups, slots, width), BF16)
    by_member = pltpu.VMEM((groups, MEMBERS, cap, width), BF16)
    facts = pltpu.VMEM((groups, 32, LANES), BF16)
    return pl.pallas_call(
        functools.partial(kernel, groups, cap),
        out_shape=jax.ShapeDtypeStruct((tok, width), BF16),
        in_specs=[hbm] * 7,
        out_specs=vmem,
        scratch_shapes=[
            pltpu.VMEM((2, tok), jnp.int32), pltpu.VMEM((2, tok), F32),
            pltpu.VMEM((tok, width), BF16), pltpu.VMEM((1, width), F32),
            pltpu.VMEM((width, ff), BF16), pltpu.VMEM((width, ff), BF16), pltpu.VMEM((ff, width), BF16),
            pltpu.VMEM((tok, width), BF16),
            by_group, facts, by_group, facts, by_member, by_member,
            pltpu.VMEM((MEMBERS * cap, ff), BF16),
            by_member, by_member, by_group, by_group,
            dma((3 + tok // min(tok, 64),)), dma((3,)), pltpu.SemaphoreType.REGULAR((groups.bit_length(),)),
            dma((groups,)), dma((groups,)), dma((groups,)), dma((groups,)),
            dma((groups, MEMBERS)), dma((groups, MEMBERS)), dma((groups, MEMBERS)), dma((groups, MEMBERS)),
            dma((groups,)), dma((groups,)),
        ],
        compiler_params=pltpu.CompilerParams(
            collective_id=0, has_side_effects=True, vmem_limit_bytes=58 * 1024 * 1024
        ),
    )(expert_ids.T, gates.T, tokens, norm_gain.reshape(1, width), w_gate, w_up, w_down)


def solution(mesh):
    return jax.shard_map(
        shards,
        mesh=mesh,
        in_specs=(
            P("ep", None),
            P(),
            P("ep", None),
            P("ep", None),
            P("ep", None, None),
            P("ep", None, None),
            P("ep", None, None),
        ),
        out_specs=P("ep", None),
        check_vma=False,
    )
```

```python
import functools

import jax
import jax.numpy as jnp
from jax import lax
from jax.experimental import pallas as pl
from jax.experimental.pallas import tpu as pltpu
from jax.sharding import PartitionSpec as P

EPS = 1e-06
MEMBERS = 4
LANES = 128
MESH = pl.DeviceIdType.MESH
F32 = jnp.float32
BF16 = jnp.bfloat16


def xor(a, b, count):
    total, bit = 0, 1
    while bit < count:
        total = total + ((a // bit + b // bit) % 2) * bit
        bit *= 2
    return total


def bits(i):
    return bin(i).count("1")


def halves(groups):
    half = groups // 2
    upper = sorted(range(half, groups), key=lambda i: (bits(i), -i))
    lower = sorted(range(1, half), key=lambda i: (bits(i), i))
    return upper, lower


def send_order(groups, distance):
    upper, lower = ([i for i in items if bits(i) == distance] for items in halves(groups))
    if distance == 1:
        return lower + upper
    order = []
    while upper or lower:
        order += upper[:1] + lower[:1]
        upper, lower = upper[1:], lower[1:]
    return order


def plan(groups):
    upper, lower = halves(groups)
    near = [i for i in lower if bits(i) == 1]
    rest = [i for i in lower if bits(i) > 1]
    steps, waiting = [], []

    def select(*items):
        steps.extend((0, i) for i in items)

    def mix(keep):
        while len(waiting) > keep:
            steps.append((1, waiting.pop(0)))

    def output(*items):
        steps.extend((2, i) for i in items)
        waiting.extend(items)

    select(0, *near, upper[0])
    output(near[0])
    select(upper[1])
    output(upper[0], *near[1:])
    for before, i in zip(upper[1:], upper[2:]):
        select(i)
        mix(1)
        output(before)
    mix(1)
    select(*rest)
    output(upper[-1])
    mix(1)
    output(*rest, 0)
    mix(0)

    rows, last = [], 2
    for kind, item in steps:
        if kind <= last:
            rows.append([-1, -1, -1])
        rows[-1][kind] = item
        last = kind
    return [list(column) for column in zip(*rows)]


PARTS = 2


def entry(table, t):
    return sum(jnp.where(t == k, value, 0) for k, value in enumerate(table) if value)


def merge_rows(block):
    parts, rows, width = block.shape
    if rows % 16 == 0:
        return block.reshape(parts * rows, width)
    return block.astype(F32).reshape(parts * rows, width).astype(BF16)


def split_rows(block, parts):
    rows, width = block.shape
    return block.reshape(parts, rows // parts, width).astype(BF16)


def chunks(width, size):
    size = min(width, size)
    return [slice(start, start + size) for start in range(0, width, size)]


def dot(a, b):
    return jnp.dot(a, b, preferred_element_type=F32)


def kernel(
    groups, cap,
    ids_hbm, gates_hbm, tokens_hbm, gain_hbm, wg_hbm, wu_hbm, wd_hbm, out_ref,
    spread_ref,
    ids_ref, gates_ref, tokens_ref, gain_ref, wg, wu, wd, normed, pack, pack_meta, blk, meta, sel, rows, hidden, outs, obuf, comb, back,
    in_sem, w_sem, near_sem, s1_send, s1_recv, m_send, m_recv, s2_send, s2_recv, r2_send, r2_recv, r1_send, r1_recv,
):
    tok, width = tokens_ref.shape
    ff = wg.shape[1]
    slots = 2 * cap
    experts = groups * MEMBERS
    me = lax.axis_index("ep")
    group, member = me // MEMBERS, me % MEMBERS

    def far(i):
        return xor(group, i, groups) * MEMBERS + member

    def near(k):
        return group * MEMBERS + xor(member, k, MEMBERS)

    distances = bits(groups - 1)
    barrier = pltpu.get_barrier_semaphore()
    for k in range(1, MEMBERS):
        pl.semaphore_signal(barrier, inc=1, device_id=(near(k),), device_id_type=MESH)
    for b in range(distances):
        pl.semaphore_signal(barrier, inc=1, device_id=(far(2**b),), device_id_type=MESH)

    block = min(tok, 64)
    small = [
        pltpu.make_async_copy(src, dst, in_sem.at[k])
        for k, (src, dst) in enumerate(((ids_hbm, ids_ref), (gates_hbm, gates_ref), (gain_hbm, gain_ref)))
    ]
    token_loads = [
        pltpu.make_async_copy(
            tokens_hbm.at[pl.ds(r, block)], tokens_ref.at[pl.ds(r, block)], in_sem.at[3 + r // block]
        )
        for r in range(0, tok, block)
    ]
    loads = [
        pltpu.make_async_copy(src.at[0], dst, w_sem.at[k])
        for k, (src, dst) in enumerate(((wg_hbm, wg), (wu_hbm, wu), (wd_hbm, wd)))
    ]
    for load in small + token_loads + loads:
        load.start()
    for load in small:
        load.wait()

    ids = ids_ref[...]
    first, second = ids[0:1, :], ids[1:2, :]
    before = (
        lax.broadcasted_iota(jnp.int32, (tok, tok), 0) < lax.broadcasted_iota(jnp.int32, (tok, tok), 1)
    ).astype(F32).astype(BF16)
    expert_iota = lax.broadcasted_iota(jnp.int32, (experts, tok), 0)
    is_first = (expert_iota == first).astype(F32)
    is_second = (expert_iota == second).astype(F32)
    earlier = dot((is_first + is_second).astype(BF16), before)
    place_first = jnp.sum(earlier * is_first, axis=0, keepdims=True) + 1.0
    place_second = jnp.sum(earlier * is_second, axis=0, keepdims=True) + 1.0
    token_group = first // MEMBERS
    group_rows = max(groups, 8)
    is_group = (lax.broadcasted_iota(jnp.int32, (group_rows, tok), 0) == token_group).astype(F32)
    slot = jnp.sum(dot(is_group.astype(BF16), before) * is_group, axis=0, keepdims=True).astype(jnp.int32)
    step_of = xor(token_group, jnp.full_like(token_group, group), groups)
    key = step_of * slots + slot

    local_first, local_second = first % MEMBERS, second % MEMBERS
    gates = gates_ref[...]
    gate_high = gates.astype(BF16).astype(F32)
    gate_low = (gates - gate_high).astype(BF16).astype(F32)

    def member_rows(of_first, of_second):
        m = lax.broadcasted_iota(jnp.int32, (8, tok), 0)
        return jnp.where(m == local_first, of_first, 0.0) + jnp.where(m == local_second, of_second, 0.0)

    facts = jnp.concatenate(
        [
            member_rows(place_first, place_second),
            member_rows(gate_high[0:1, :], gate_high[1:2, :]),
            member_rows(gate_low[0:1, :], gate_low[1:2, :]),
            jnp.zeros((8, tok), F32),
        ],
        axis=0,
    ).astype(BF16)
    pick_iota = lax.broadcasted_iota(jnp.int32, (groups * slots, tok), 0)
    picked = (pick_iota == key).astype(F32).astype(BF16)
    wide_iota = lax.broadcasted_iota(jnp.int32, (groups * LANES, tok), 0)
    wide = (wide_iota == step_of * LANES + slot).astype(F32).astype(BF16)
    told = lax.dot_general(
        facts, wide, (((1,), (1,)), ((), ())), preferred_element_type=F32
    ).astype(BF16)
    meta[0] = told[:, :LANES]
    for i in range(1, groups):
        pack_meta[i] = told[:, i * LANES : (i + 1) * LANES]
    for r in range(0, tok, block):
        token_loads[r // block].wait()
        lines = pl.ds(r, block)
        floats = tokens_ref[lines, :].astype(F32)
        inverse = lax.rsqrt(jnp.mean(floats * floats, axis=-1, keepdims=True) + EPS)
        normed[lines, :] = (floats * inverse * gain_ref[...]).astype(BF16)

    part = width // PARTS
    for h in range(PARTS):
        for cols in chunks(part, 256):
            source = slice(h * part + cols.start, h * part + cols.stop)
            packed = split_rows(dot(picked, normed[:, source]), groups)
            blk[0, h, :, cols] = packed[0]
            pack[1:, h, :, cols] = packed[1:]

    def s1_copy(i, h):
        return pltpu.make_async_remote_copy(
            src_ref=pack.at[i, h], dst_ref=blk.at[i, h], send_sem=s1_send.at[0], recv_sem=s1_recv.at[i, h],
            device_id=(far(i),), device_id_type=MESH,
        )

    def meta_copy(i):
        return pltpu.make_async_remote_copy(
            src_ref=pack_meta.at[i], dst_ref=meta.at[i], send_sem=m_send.at[0], recv_sem=m_recv.at[i],
            device_id=(far(i),), device_id_type=MESH,
        )

    def s2_copy(i, h, k):
        peer = xor(member, k, MEMBERS)
        return pltpu.make_async_remote_copy(
            src_ref=sel.at[i, h, peer], dst_ref=rows.at[i, h, member],
            send_sem=s2_send.at[0], recv_sem=s2_recv.at[i],
            device_id=(near(k),), device_id_type=MESH,
        )

    def r2_copy(i, h, k):
        peer = xor(member, k, MEMBERS)
        return pltpu.make_async_remote_copy(
            src_ref=outs.at[i, h, peer], dst_ref=obuf.at[i, h, member],
            send_sem=r2_send.at[0], recv_sem=r2_recv.at[i, h],
            device_id=(near(k),), device_id_type=MESH,
        )

    def r1_copy(i, h):
        return pltpu.make_async_remote_copy(
            src_ref=comb.at[i, h], dst_ref=back.at[i, h], send_sem=r1_send.at[0], recv_sem=r1_recv.at[0],
            device_id=(far(i),), device_id_type=MESH,
        )

    def landed(ref, sem):
        pltpu.make_async_copy(ref, ref, sem).wait()

    def send(distance):
        if distance == 1:
            pl.semaphore_wait(barrier, MEMBERS - 1 + distances)
        else:
            pl.semaphore_wait(near_sem.at[distance], distances)
        if distance < distances:
            for b in range(distances):
                pl.semaphore_signal(
                    near_sem.at[distance + 1], inc=1, device_id=(far(2**b),), device_id_type=MESH
                )
        for i in send_order(groups, distance):
            meta_copy(i).start()
            for h in range(PARTS):
                s1_copy(i, h).start()

    send(1)

    place_iota = lax.broadcasted_iota(jnp.int32, (cap, LANES), 0).astype(F32) + 1.0

    def one_hots(i):
        info = meta[i].astype(F32)
        return info, [(place_iota == info[m : m + 1, :]) for m in range(MEMBERS)]

    def select(i):
        @pl.when(i > 0)
        def _():
            meta_copy(i).wait_recv()

        _, hots = one_hots(i)
        pick = jnp.concatenate([h.astype(F32) for h in hots], axis=0).astype(BF16)[:, :slots]
        for h in range(PARTS):
            @pl.when(i > 0)
            def _():
                s1_copy(i, h).wait_recv()

            for cols in chunks(part, 512):
                sel[i, h, :, :, cols] = split_rows(dot(pick, blk[i, h, :, cols]), MEMBERS)
            for k in (2, 3, 1):
                s2_copy(i, h, k).start()
            rows[i, h, member] = sel[i, h, member]

    def ffn(i, is_first):
        @pl.when(is_first)
        def _():
            for load in loads:
                load.wait()

        landed(rows.at[i, :, 1:], s2_recv.at[i])
        xs = [merge_rows(rows[i, h]) for h in range(PARTS)]
        for cols in chunks(ff, 256):
            gate_part = sum(dot(x, wg[h * part : (h + 1) * part, cols]) for h, x in enumerate(xs))
            up_part = sum(dot(x, wu[h * part : (h + 1) * part, cols]) for h, x in enumerate(xs))
            hidden[:, cols] = (gate_part / (1.0 + jnp.exp(-gate_part)) * up_part).astype(BF16)
        hid = hidden[...]
        for h in range(PARTS):
            for cols in chunks(part, 256):
                source = slice(h * part + cols.start, h * part + cols.stop)
                outs[i, h, :, :, cols] = split_rows(dot(hid, wd[:, source]), MEMBERS)
            for k in (2, 3, 1):
                r2_copy(i, h, k).start()
            obuf[i, h, member] = outs[i, h, member]

    def mix(i):
        info, hots = one_hots(i)

        def weights(row):
            parts = [jnp.where(hots[m], info[row + m : row + m + 1, :], 0.0) for m in range(MEMBERS)]
            return jnp.concatenate(parts, axis=0).T[:slots].astype(BF16)

        high, low = weights(8), weights(16)

        def mixed(h, cols):
            values = merge_rows(obuf[i, h, :, :, cols])
            return (dot(high, values) + dot(low, values)).astype(BF16)

        for h in range(PARTS):
            landed(obuf.at[i, h, 1:], r2_recv.at[i, h])

            @pl.when(i == 0)
            def _():
                for cols in chunks(part, 512):
                    back[0, h, :, cols] = mixed(h, cols)

            @pl.when(i > 0)
            def _():
                for cols in chunks(part, 512):
                    comb[i, h, :, cols] = mixed(h, cols)
                r1_copy(i, h).start()

    key_column = jnp.broadcast_to(key.astype(F32), (LANES, tok)).T[:, 0:1].astype(jnp.int32)
    spread_ref[...] = (
        lax.broadcasted_iota(jnp.int32, (tok, groups * slots), 1) == key_column
    ).astype(F32).astype(BF16)

    selects, mixes, outputs = plan(groups)
    first_output = next(t for t, i in enumerate(outputs) if i >= 0)

    @pl.loop(0, len(selects))
    def _(t):
        to_select, to_mix, to_output = entry(selects, t), entry(mixes, t), entry(outputs, t)

        @pl.when(to_select >= 0)
        def _():
            select(to_select)

        for d in range(2, distances + 1):
            @pl.when(t == d - 2)
            def _():
                send(d)

        @pl.when(to_mix >= 0)
        def _():
            mix(to_mix)

        @pl.when(to_output >= 0)
        def _():
            ffn(to_output, t == first_output)

    landed(pack.at[1:], s1_send.at[0])
    landed(pack_meta.at[1:], m_send.at[0])
    landed(sel.at[:, :, 1:], s2_send.at[0])
    landed(outs.at[:, :, 1:], r2_send.at[0])
    landed(comb.at[1:], r1_send.at[0])
    landed(back.at[1:], r1_recv.at[0])
    for h in range(PARTS):
        for cols in chunks(part, 512):
            target = pl.ds(h * part + cols.start, cols.stop - cols.start)
            out_ref[:, target] = dot(spread_ref[...], merge_rows(back[:, h, :, cols])).astype(BF16)


def shards(tokens, norm_gain, expert_ids, gates, w_gate, w_up, w_down):
    tok, width = tokens.shape
    ff = w_gate.shape[2]
    experts = lax.axis_size("ep")
    groups = experts // MEMBERS
    cap = 2 * ((2 * tok + experts - 1) // experts)
    slots = 2 * cap
    hbm = pl.BlockSpec(memory_space=pltpu.HBM)
    dma = pltpu.SemaphoreType.DMA
    by_group = pltpu.VMEM((groups, PARTS, slots, width // PARTS), BF16)
    by_member = pltpu.VMEM((groups, PARTS, MEMBERS, cap, width // PARTS), BF16)
    facts = pltpu.VMEM((groups, 32, LANES), BF16)
    return pl.pallas_call(
        functools.partial(kernel, groups, cap),
        out_shape=jax.ShapeDtypeStruct((tok, width), BF16),
        in_specs=[hbm] * 7,
        out_specs=pl.BlockSpec(memory_space=pltpu.VMEM),
        scratch_shapes=[
            pltpu.VMEM((tok, groups * slots), BF16),
            pltpu.VMEM((2, tok), jnp.int32), pltpu.VMEM((2, tok), F32),
            pltpu.VMEM((tok, width), BF16), pltpu.VMEM((1, width), F32),
            pltpu.VMEM((width, ff), BF16), pltpu.VMEM((width, ff), BF16), pltpu.VMEM((ff, width), BF16),
            pltpu.VMEM((tok, width), BF16),
            by_group, facts, by_group, facts, by_member, by_member,
            pltpu.VMEM((MEMBERS * cap, ff), BF16),
            by_member, by_member, by_group, by_group,
            dma((3 + tok // min(tok, 64),)), dma((3,)), pltpu.SemaphoreType.REGULAR((groups.bit_length(),)),
            dma((1,)), dma((groups, PARTS)), dma((1,)), dma((groups,)),
            dma((1,)), dma((groups,)), dma((1,)), dma((groups, PARTS)), dma((1,)), dma((1,)),
        ],
        compiler_params=pltpu.CompilerParams(
            collective_id=0, has_side_effects=True, vmem_limit_bytes=50 * 1024 * 1024
        ),
    )(*[pltpu.with_memory_space_constraint(a, pltpu.HBM) for a in (expert_ids.T, gates.T, tokens, norm_gain.reshape(1, width), w_gate, w_up, w_down)])


def solution(mesh):
    return jax.shard_map(
        shards,
        mesh=mesh,
        in_specs=(
            P("ep", None),
            P(),
            P("ep", None),
            P("ep", None),
            P("ep", None, None),
            P("ep", None, None),
            P("ep", None, None),
        ),
        out_specs=P("ep", None),
        check_vma=False,
    )
```

```python
import functools

import jax
import jax.numpy as jnp
from jax import lax
from jax.experimental import pallas as pl
from jax.experimental.pallas import tpu as pltpu
from jax.sharding import PartitionSpec as P

EPS = 1e-06
MEMBERS = 4
LANES = 128
MESH = pl.DeviceIdType.MESH
F32 = jnp.float32
BF16 = jnp.bfloat16


def xor(a, b, count):
    total, bit = 0, 1
    while bit < count:
        total = total + ((a // bit + b // bit) % 2) * bit
        bit *= 2
    return total


def bits(i):
    return bin(i).count("1")


def halves(groups):
    half = groups // 2
    upper = sorted(range(half, groups), key=lambda i: (bits(i), -i))
    lower = sorted(range(1, half), key=lambda i: (bits(i), i))
    return upper, lower


def send_order(groups, distance):
    upper, lower = ([i for i in items if bits(i) == distance] for items in halves(groups))
    if distance == 1:
        return lower + upper
    order = []
    while upper or lower:
        order += upper[:1] + lower[:1]
        upper, lower = upper[1:], lower[1:]
    return order


def plan(groups):
    upper, lower = halves(groups)
    near = [i for i in lower if bits(i) == 1]
    rest = [i for i in lower if bits(i) > 1]
    steps, waiting = [], []

    def select(*items):
        steps.extend((0, i) for i in items)

    def mix(keep):
        while len(waiting) > keep:
            steps.append((1, waiting.pop(0)))

    def output(*items):
        steps.extend((2, i) for i in items)
        waiting.extend(items)

    select(0, *near, upper[0])
    output(near[0])
    select(upper[1])
    output(upper[0], *near[1:])
    for before, i in zip(upper[1:], upper[2:]):
        select(i)
        mix(1)
        output(before)
    mix(1)
    select(*rest)
    output(upper[-1])
    mix(1)
    output(*rest, 0)
    mix(0)

    rows, last = [], 2
    for kind, item in steps:
        if kind <= last:
            rows.append([-1, -1, -1])
        rows[-1][kind] = item
        last = kind
    return [list(column) for column in zip(*rows)]


PARTS = 2


def entry(table, t):
    return sum(jnp.where(t == k, value, 0) for k, value in enumerate(table) if value)


def merge_rows(block):
    parts, rows, width = block.shape
    if rows % 16 == 0:
        return block.reshape(parts * rows, width)
    return block.astype(F32).reshape(parts * rows, width).astype(BF16)


def split_rows(block, parts):
    rows, width = block.shape
    return block.reshape(parts, rows // parts, width).astype(BF16)


def chunks(width, size):
    size = min(width, size)
    return [slice(start, start + size) for start in range(0, width, size)]


def dot(a, b):
    return jnp.dot(a, b, preferred_element_type=F32)


def kernel(
    groups, cap,
    ids_hbm, gates_hbm, tokens_hbm, gain_hbm, wg_hbm, wu_hbm, wd_hbm, out_ref,
    spread_ref,
    ids_ref, gates_ref, tokens_ref, gain_ref, wg, wu, wd, normed, pack, pack_meta, blk, meta, sel, rows, hidden, outs, obuf, comb, back,
    in_sem, w_sem, near_sem, s1_send, s1_recv, m_send, m_recv, s2_send, s2_recv, r2_send, r2_recv, r1_send, r1_recv,
):
    tok, width = tokens_ref.shape
    ff = wg.shape[1]
    slots = 2 * cap
    experts = groups * MEMBERS
    me = lax.axis_index("ep")
    group, member = me // MEMBERS, me % MEMBERS

    def far(i):
        return xor(group, i, groups) * MEMBERS + member

    def near(k):
        return group * MEMBERS + xor(member, k, MEMBERS)

    distances = bits(groups - 1)
    barrier = pltpu.get_barrier_semaphore()
    for k in range(1, MEMBERS):
        pl.semaphore_signal(barrier, inc=1, device_id=(near(k),), device_id_type=MESH)
    for b in range(distances):
        pl.semaphore_signal(barrier, inc=1, device_id=(far(2**b),), device_id_type=MESH)

    block = min(tok, 64)
    small = [
        pltpu.make_async_copy(src, dst, in_sem.at[k])
        for k, (src, dst) in enumerate(((ids_hbm, ids_ref), (gates_hbm, gates_ref), (gain_hbm, gain_ref)))
    ]
    token_loads = [
        pltpu.make_async_copy(
            tokens_hbm.at[pl.ds(r, block)], tokens_ref.at[pl.ds(r, block)], in_sem.at[3 + r // block]
        )
        for r in range(0, tok, block)
    ]
    loads = [
        pltpu.make_async_copy(src.at[0], dst, w_sem.at[k])
        for k, (src, dst) in enumerate(((wg_hbm, wg), (wu_hbm, wu), (wd_hbm, wd)))
    ]
    for load in small + token_loads:
        load.start()
    for load in small:
        load.wait()

    ids = ids_ref[...]
    first, second = ids[0:1, :], ids[1:2, :]
    before = (
        lax.broadcasted_iota(jnp.int32, (tok, tok), 0) < lax.broadcasted_iota(jnp.int32, (tok, tok), 1)
    ).astype(F32).astype(BF16)
    expert_iota = lax.broadcasted_iota(jnp.int32, (experts, tok), 0)
    is_first = (expert_iota == first).astype(F32)
    is_second = (expert_iota == second).astype(F32)
    earlier = dot((is_first + is_second).astype(BF16), before)
    place_first = jnp.sum(earlier * is_first, axis=0, keepdims=True) + 1.0
    place_second = jnp.sum(earlier * is_second, axis=0, keepdims=True) + 1.0
    token_group = first // MEMBERS
    group_rows = max(groups, 8)
    is_group = (lax.broadcasted_iota(jnp.int32, (group_rows, tok), 0) == token_group).astype(F32)
    slot = jnp.sum(dot(is_group.astype(BF16), before) * is_group, axis=0, keepdims=True).astype(jnp.int32)
    step_of = xor(token_group, jnp.full_like(token_group, group), groups)
    key = step_of * slots + slot

    local_first, local_second = first % MEMBERS, second % MEMBERS
    gates = gates_ref[...]
    gate_high = gates.astype(BF16).astype(F32)
    gate_low = (gates - gate_high).astype(BF16).astype(F32)

    def member_rows(of_first, of_second):
        m = lax.broadcasted_iota(jnp.int32, (8, tok), 0)
        return jnp.where(m == local_first, of_first, 0.0) + jnp.where(m == local_second, of_second, 0.0)

    facts = jnp.concatenate(
        [
            member_rows(place_first, place_second),
            member_rows(gate_high[0:1, :], gate_high[1:2, :]),
            member_rows(gate_low[0:1, :], gate_low[1:2, :]),
            jnp.zeros((8, tok), F32),
        ],
        axis=0,
    ).astype(BF16)
    pick_iota = lax.broadcasted_iota(jnp.int32, (groups * slots, tok), 0)
    picked = (pick_iota == key).astype(F32).astype(BF16)
    wide_iota = lax.broadcasted_iota(jnp.int32, (groups * LANES, tok), 0)
    wide = (wide_iota == step_of * LANES + slot).astype(F32).astype(BF16)
    told = lax.dot_general(
        facts, wide, (((1,), (1,)), ((), ())), preferred_element_type=F32
    ).astype(BF16)
    meta[0] = told[:, :LANES]
    for i in range(1, groups):
        pack_meta[i] = told[:, i * LANES : (i + 1) * LANES]
    for r in range(0, tok, min(tok, 16)):
        if r % block == 0:
            token_loads[r // block].wait()
        lines = pl.ds(r, min(tok, 16))
        floats = tokens_ref[lines, :].astype(F32)
        inverse = lax.rsqrt(jnp.mean(floats * floats, axis=-1, keepdims=True) + EPS)
        normed[lines, :] = (floats * inverse * gain_ref[...]).astype(BF16)

    for load in loads:
        load.start()

    part = width // PARTS
    for h in range(PARTS):
        for cols in chunks(part, 256):
            source = slice(h * part + cols.start, h * part + cols.stop)
            packed = split_rows(dot(picked, normed[:, source]), groups)
            blk[0, h, :, cols] = packed[0]
            pack[1:, h, :, cols] = packed[1:]

    def s1_copy(i, h):
        return pltpu.make_async_remote_copy(
            src_ref=pack.at[i, h], dst_ref=blk.at[i, h], send_sem=s1_send.at[0], recv_sem=s1_recv.at[i, h],
            device_id=(far(i),), device_id_type=MESH,
        )

    def meta_copy(i):
        return pltpu.make_async_remote_copy(
            src_ref=pack_meta.at[i], dst_ref=meta.at[i], send_sem=m_send.at[0], recv_sem=m_recv.at[i],
            device_id=(far(i),), device_id_type=MESH,
        )

    def s2_copy(i, h, k):
        peer = xor(member, k, MEMBERS)
        return pltpu.make_async_remote_copy(
            src_ref=sel.at[i, h, peer], dst_ref=rows.at[i, h, member],
            send_sem=s2_send.at[0], recv_sem=s2_recv.at[i],
            device_id=(near(k),), device_id_type=MESH,
        )

    def r2_copy(i, h, k):
        peer = xor(member, k, MEMBERS)
        return pltpu.make_async_remote_copy(
            src_ref=outs.at[i, h, peer], dst_ref=obuf.at[i, h, member],
            send_sem=r2_send.at[0], recv_sem=r2_recv.at[i, h],
            device_id=(near(k),), device_id_type=MESH,
        )

    def r1_copy(i, h):
        return pltpu.make_async_remote_copy(
            src_ref=comb.at[i, h], dst_ref=back.at[i, h], send_sem=r1_send.at[0], recv_sem=r1_recv.at[0],
            device_id=(far(i),), device_id_type=MESH,
        )

    def landed(ref, sem):
        pltpu.make_async_copy(ref, ref, sem).wait()

    def send(distance):
        if distance == 1:
            pl.semaphore_wait(barrier, MEMBERS - 1 + distances)
        else:
            pl.semaphore_wait(near_sem.at[distance], distances)
        if distance < distances:
            for b in range(distances):
                pl.semaphore_signal(
                    near_sem.at[distance + 1], inc=1, device_id=(far(2**b),), device_id_type=MESH
                )
        for i in send_order(groups, distance):
            meta_copy(i).start()
            for h in range(PARTS):
                s1_copy(i, h).start()

    send(1)

    place_iota = lax.broadcasted_iota(jnp.int32, (cap, LANES), 0).astype(F32) + 1.0

    def one_hots(i):
        info = meta[i].astype(F32)
        return info, [(place_iota == info[m : m + 1, :]) for m in range(MEMBERS)]

    def select(i):
        @pl.when(i > 0)
        def _():
            meta_copy(i).wait_recv()

        _, hots = one_hots(i)
        pick = jnp.concatenate([h.astype(F32) for h in hots], axis=0).astype(BF16)[:, :slots]
        for h in range(PARTS):
            @pl.when(i > 0)
            def _():
                s1_copy(i, h).wait_recv()

            for cols in chunks(part, 512):
                sel[i, h, :, :, cols] = split_rows(dot(pick, blk[i, h, :, cols]), MEMBERS)
            for k in (2, 3, 1):
                s2_copy(i, h, k).start()
            rows[i, h, member] = sel[i, h, member]

    def ffn(i, is_first):
        @pl.when(is_first)
        def _():
            for load in loads:
                load.wait()

        landed(rows.at[i, :, 1:], s2_recv.at[i])
        xs = [merge_rows(rows[i, h]) for h in range(PARTS)]
        for cols in chunks(ff, 256):
            gate_part = sum(dot(x, wg[h * part : (h + 1) * part, cols]) for h, x in enumerate(xs))
            up_part = sum(dot(x, wu[h * part : (h + 1) * part, cols]) for h, x in enumerate(xs))
            hidden[:, cols] = (gate_part / (1.0 + jnp.exp(-gate_part)) * up_part).astype(BF16)
        hid = hidden[...]
        for h in range(PARTS):
            for cols in chunks(part, 256):
                source = slice(h * part + cols.start, h * part + cols.stop)
                outs[i, h, :, :, cols] = split_rows(dot(hid, wd[:, source]), MEMBERS)
            for k in (2, 3, 1):
                r2_copy(i, h, k).start()
            obuf[i, h, member] = outs[i, h, member]

    def mix(i):
        info, hots = one_hots(i)

        def weights(row):
            parts = [jnp.where(hots[m], info[row + m : row + m + 1, :], 0.0) for m in range(MEMBERS)]
            return jnp.concatenate(parts, axis=0).T[:slots].astype(BF16)

        high, low = weights(8), weights(16)

        def mixed(h, cols):
            values = merge_rows(obuf[i, h, :, :, cols])
            return (dot(high, values) + dot(low, values)).astype(BF16)

        for h in range(PARTS):
            landed(obuf.at[i, h, 1:], r2_recv.at[i, h])

            @pl.when(i == 0)
            def _():
                for cols in chunks(part, 512):
                    back[0, h, :, cols] = mixed(h, cols)

            @pl.when(i > 0)
            def _():
                for cols in chunks(part, 512):
                    comb[i, h, :, cols] = mixed(h, cols)
                r1_copy(i, h).start()

    selects, mixes, outputs = plan(groups)
    first_output = next(t for t, i in enumerate(outputs) if i >= 0)

    @pl.loop(0, len(selects))
    def _(t):
        to_select, to_mix, to_output = entry(selects, t), entry(mixes, t), entry(outputs, t)

        @pl.when(to_select >= 0)
        def _():
            select(to_select)

        for d in range(2, distances + 1):
            @pl.when(t == d - 2)
            def _():
                send(d)

        @pl.when(t == 1)
        def _():
            key_column = jnp.broadcast_to(key.astype(F32), (LANES, tok)).T[:, 0:1].astype(jnp.int32)
            spread_ref[...] = (
                lax.broadcasted_iota(jnp.int32, (tok, groups * slots), 1) == key_column
            ).astype(F32).astype(BF16)

        @pl.when(to_mix >= 0)
        def _():
            mix(to_mix)

        @pl.when(to_output >= 0)
        def _():
            ffn(to_output, t == first_output)

    landed(pack.at[1:], s1_send.at[0])
    landed(pack_meta.at[1:], m_send.at[0])
    landed(sel.at[:, :, 1:], s2_send.at[0])
    landed(outs.at[:, :, 1:], r2_send.at[0])
    landed(comb.at[1:], r1_send.at[0])
    landed(back.at[1:], r1_recv.at[0])
    for h in range(PARTS):
        for cols in chunks(part, 512):
            target = pl.ds(h * part + cols.start, cols.stop - cols.start)
            out_ref[:, target] = dot(spread_ref[...], merge_rows(back[:, h, :, cols])).astype(BF16)


def shards(tokens, norm_gain, expert_ids, gates, w_gate, w_up, w_down):
    tok, width = tokens.shape
    ff = w_gate.shape[2]
    experts = lax.axis_size("ep")
    groups = experts // MEMBERS
    cap = 2 * ((2 * tok + experts - 1) // experts)
    slots = 2 * cap
    hbm = pl.BlockSpec(memory_space=pltpu.HBM)
    dma = pltpu.SemaphoreType.DMA
    by_group = pltpu.VMEM((groups, PARTS, slots, width // PARTS), BF16)
    by_member = pltpu.VMEM((groups, PARTS, MEMBERS, cap, width // PARTS), BF16)
    facts = pltpu.VMEM((groups, 32, LANES), BF16)
    return pl.pallas_call(
        functools.partial(kernel, groups, cap),
        out_shape=jax.ShapeDtypeStruct((tok, width), BF16),
        in_specs=[hbm] * 7,
        out_specs=pl.BlockSpec(memory_space=pltpu.VMEM),
        scratch_shapes=[
            pltpu.VMEM((tok, groups * slots), BF16),
            pltpu.VMEM((2, tok), jnp.int32), pltpu.VMEM((2, tok), F32),
            pltpu.VMEM((tok, width), BF16), pltpu.VMEM((1, width), F32),
            pltpu.VMEM((width, ff), BF16), pltpu.VMEM((width, ff), BF16), pltpu.VMEM((ff, width), BF16),
            pltpu.VMEM((tok, width), BF16),
            by_group, facts, by_group, facts, by_member, by_member,
            pltpu.VMEM((MEMBERS * cap, ff), BF16),
            by_member, by_member, by_group, by_group,
            dma((3 + tok // min(tok, 64),)), dma((3,)), pltpu.SemaphoreType.REGULAR((groups.bit_length(),)),
            dma((1,)), dma((groups, PARTS)), dma((1,)), dma((groups,)),
            dma((1,)), dma((groups,)), dma((1,)), dma((groups, PARTS)), dma((1,)), dma((1,)),
        ],
        compiler_params=pltpu.CompilerParams(
            collective_id=0, has_side_effects=True, vmem_limit_bytes=50 * 1024 * 1024
        ),
    )(*[pltpu.with_memory_space_constraint(a, pltpu.HBM) for a in (expert_ids.T, gates.T, tokens, norm_gain.reshape(1, width), w_gate, w_up, w_down)])


def solution(mesh):
    return jax.shard_map(
        shards,
        mesh=mesh,
        in_specs=(
            P("ep", None),
            P(),
            P("ep", None),
            P("ep", None),
            P("ep", None, None),
            P("ep", None, None),
            P("ep", None, None),
        ),
        out_specs=P("ep", None),
        check_vma=False,
    )
```

```python
import functools

import jax
import jax.numpy as jnp
from jax import lax
from jax.experimental import pallas as pl
from jax.experimental.pallas import tpu as pltpu
from jax.sharding import PartitionSpec as P

EPS = 1e-06
MEMBERS = 4
LANES = 128
MESH = pl.DeviceIdType.MESH
F32 = jnp.float32
BF16 = jnp.bfloat16


def xor(a, b, count):
    total, bit = 0, 1
    while bit < count:
        total = total + ((a // bit + b // bit) % 2) * bit
        bit *= 2
    return total


def bits(i):
    return bin(i).count("1")


def halves(groups):
    half = groups // 2
    upper = sorted(range(half, groups), key=lambda i: (bits(i), -i))
    lower = sorted(range(1, half), key=lambda i: (bits(i), i))
    return upper, lower


def send_order(groups, distance):
    upper, lower = ([i for i in items if bits(i) == distance] for items in halves(groups))
    if distance == 1:
        return lower + upper
    order = []
    while upper or lower:
        order += upper[:1] + lower[:1]
        upper, lower = upper[1:], lower[1:]
    return order


def plan(groups, outer):
    upper, lower = halves(groups)
    near = [i for i in lower if bits(i) == 1]
    rest = [i for i in lower if bits(i) > 1]
    steps, waiting = [], []

    def select(*items):
        steps.extend((0, i) for i in items)

    def mix(keep):
        while len(waiting) > keep:
            steps.append((1, waiting.pop(0)))

    def output(*items):
        steps.extend((2, i) for i in items)
        waiting.extend(items)

    select(0, *near, upper[0])
    output(near[0])
    select(upper[1])
    output(upper[0])
    if outer:
        select(*rest)
    else:
        output(*near[1:])
    for before, i in zip(upper[1:], upper[2:]):
        select(i)
        mix(1)
        output(before)
    mix(1)
    if outer:
        output(*rest, upper[-1])
        mix(len(rest) + 1)
        output(*near[1:])
        mix(len(near))
        output(0)
    else:
        select(*rest)
        output(upper[-1])
        mix(1)
        output(*rest, 0)
    mix(0)

    rows, last = [], 2
    for kind, item in steps:
        if kind <= last:
            rows.append([-1, -1, -1])
        rows[-1][kind] = item
        last = kind
    return [list(column) for column in zip(*rows)]


PARTS = 2


def entry(table, t):
    return sum(jnp.where(t == k, value, 0) for k, value in enumerate(table) if value)


def merge_rows(block):
    parts, rows, width = block.shape
    if rows % 16 == 0:
        return block.reshape(parts * rows, width)
    return block.astype(F32).reshape(parts * rows, width).astype(BF16)


def split_rows(block, parts):
    rows, width = block.shape
    return block.reshape(parts, rows // parts, width).astype(BF16)


def chunks(width, size):
    size = min(width, size)
    return [slice(start, start + size) for start in range(0, width, size)]


def dot(a, b):
    return jnp.dot(a, b, preferred_element_type=F32)


def kernel(
    groups, cap,
    ids_hbm, gates_hbm, tokens_hbm, gain_hbm, wg_hbm, wu_hbm, wd_hbm, out_ref,
    spread_ref,
    ids_ref, gates_ref, tokens_ref, gain_ref, wg, wu, wd, normed, pack, pack_meta, blk, meta, sel, rows, hidden, outs, obuf, comb, back,
    in_sem, w_sem, near_sem, s1_send, s1_recv, m_send, m_recv, s2_send, s2_recv, r2_send, r2_recv, r1_send, r1_recv,
):
    tok, width = tokens_ref.shape
    ff = wg.shape[1]
    slots = 2 * cap
    experts = groups * MEMBERS
    me = lax.axis_index("ep")
    group, member = me // MEMBERS, me % MEMBERS

    def far(i):
        return xor(group, i, groups) * MEMBERS + member

    def near(k):
        return group * MEMBERS + xor(member, k, MEMBERS)

    distances = bits(groups - 1)
    barrier = pltpu.get_barrier_semaphore()
    for k in range(1, MEMBERS):
        pl.semaphore_signal(barrier, inc=1, device_id=(near(k),), device_id_type=MESH)
    for b in range(distances):
        pl.semaphore_signal(barrier, inc=1, device_id=(far(2**b),), device_id_type=MESH)

    block = min(tok, 64)
    small = [
        pltpu.make_async_copy(src, dst, in_sem.at[k])
        for k, (src, dst) in enumerate(((ids_hbm, ids_ref), (gates_hbm, gates_ref), (gain_hbm, gain_ref)))
    ]
    token_loads = [
        pltpu.make_async_copy(
            tokens_hbm.at[pl.ds(r, block)], tokens_ref.at[pl.ds(r, block)], in_sem.at[3 + r // block]
        )
        for r in range(0, tok, block)
    ]
    loads = [
        pltpu.make_async_copy(src.at[0], dst, w_sem.at[k])
        for k, (src, dst) in enumerate(((wg_hbm, wg), (wu_hbm, wu), (wd_hbm, wd)))
    ]
    for load in small + token_loads:
        load.start()
    for load in small:
        load.wait()

    ids = ids_ref[...]
    first, second = ids[0:1, :], ids[1:2, :]
    before = (
        lax.broadcasted_iota(jnp.int32, (tok, tok), 0) < lax.broadcasted_iota(jnp.int32, (tok, tok), 1)
    ).astype(F32).astype(BF16)
    expert_iota = lax.broadcasted_iota(jnp.int32, (experts, tok), 0)
    is_first = (expert_iota == first).astype(F32)
    is_second = (expert_iota == second).astype(F32)
    earlier = dot((is_first + is_second).astype(BF16), before)
    place_first = jnp.sum(earlier * is_first, axis=0, keepdims=True) + 1.0
    place_second = jnp.sum(earlier * is_second, axis=0, keepdims=True) + 1.0
    token_group = first // MEMBERS
    group_rows = max(groups, 8)
    is_group = (lax.broadcasted_iota(jnp.int32, (group_rows, tok), 0) == token_group).astype(F32)
    slot = jnp.sum(dot(is_group.astype(BF16), before) * is_group, axis=0, keepdims=True).astype(jnp.int32)
    step_of = xor(token_group, jnp.full_like(token_group, group), groups)
    key = step_of * slots + slot

    local_first, local_second = first % MEMBERS, second % MEMBERS
    gates = gates_ref[...]
    gate_high = gates.astype(BF16).astype(F32)
    gate_low = (gates - gate_high).astype(BF16).astype(F32)

    def member_rows(of_first, of_second):
        m = lax.broadcasted_iota(jnp.int32, (8, tok), 0)
        return jnp.where(m == local_first, of_first, 0.0) + jnp.where(m == local_second, of_second, 0.0)

    facts = jnp.concatenate(
        [
            member_rows(place_first, place_second),
            member_rows(gate_high[0:1, :], gate_high[1:2, :]),
            member_rows(gate_low[0:1, :], gate_low[1:2, :]),
            jnp.zeros((8, tok), F32),
        ],
        axis=0,
    ).astype(BF16)
    pick_iota = lax.broadcasted_iota(jnp.int32, (groups * slots, tok), 0)
    picked = (pick_iota == key).astype(F32).astype(BF16)
    wide_iota = lax.broadcasted_iota(jnp.int32, (groups * LANES, tok), 0)
    wide = (wide_iota == step_of * LANES + slot).astype(F32).astype(BF16)
    told = lax.dot_general(
        facts, wide, (((1,), (1,)), ((), ())), preferred_element_type=F32
    ).astype(BF16)
    meta[0] = told[:, :LANES]
    for i in range(1, groups):
        pack_meta[i] = told[:, i * LANES : (i + 1) * LANES]
    for r in range(0, tok, min(tok, 16)):
        if r % block == 0:
            token_loads[r // block].wait()
        lines = pl.ds(r, min(tok, 16))
        floats = tokens_ref[lines, :].astype(F32)
        inverse = lax.rsqrt(jnp.mean(floats * floats, axis=-1, keepdims=True) + EPS)
        normed[lines, :] = (floats * inverse * gain_ref[...]).astype(BF16)

    for load in loads:
        load.start()

    part = width // PARTS
    for h in range(PARTS):
        for cols in chunks(part, 256):
            source = slice(h * part + cols.start, h * part + cols.stop)
            packed = split_rows(dot(picked, normed[:, source]), groups)
            blk[0, h, :, cols] = packed[0]
            pack[1:, h, :, cols] = packed[1:]

    def s1_copy(i, h):
        return pltpu.make_async_remote_copy(
            src_ref=pack.at[i, h], dst_ref=blk.at[i, h], send_sem=s1_send.at[0], recv_sem=s1_recv.at[i, h],
            device_id=(far(i),), device_id_type=MESH,
        )

    def meta_copy(i):
        return pltpu.make_async_remote_copy(
            src_ref=pack_meta.at[i], dst_ref=meta.at[i], send_sem=m_send.at[0], recv_sem=m_recv.at[i],
            device_id=(far(i),), device_id_type=MESH,
        )

    def s2_copy(i, h, k):
        peer = xor(member, k, MEMBERS)
        return pltpu.make_async_remote_copy(
            src_ref=sel.at[i, h, peer], dst_ref=rows.at[i, h, member],
            send_sem=s2_send.at[0], recv_sem=s2_recv.at[i],
            device_id=(near(k),), device_id_type=MESH,
        )

    def r2_copy(i, h, k):
        peer = xor(member, k, MEMBERS)
        return pltpu.make_async_remote_copy(
            src_ref=outs.at[i, h, peer], dst_ref=obuf.at[i, h, member],
            send_sem=r2_send.at[0], recv_sem=r2_recv.at[i, h],
            device_id=(near(k),), device_id_type=MESH,
        )

    def r1_copy(i, h):
        return pltpu.make_async_remote_copy(
            src_ref=comb.at[i, h], dst_ref=back.at[i, h], send_sem=r1_send.at[0], recv_sem=r1_recv.at[0],
            device_id=(far(i),), device_id_type=MESH,
        )

    def landed(ref, sem):
        pltpu.make_async_copy(ref, ref, sem).wait()

    def send(distance):
        if distance == 1:
            pl.semaphore_wait(barrier, MEMBERS - 1 + distances)
        else:
            pl.semaphore_wait(near_sem.at[distance], distances)
        if distance < distances:
            for b in range(distances):
                pl.semaphore_signal(
                    near_sem.at[distance + 1], inc=1, device_id=(far(2**b),), device_id_type=MESH
                )
        for i in send_order(groups, distance):
            meta_copy(i).start()
            for h in range(PARTS):
                s1_copy(i, h).start()

    send(1)

    place_iota = lax.broadcasted_iota(jnp.int32, (cap, LANES), 0).astype(F32) + 1.0

    def one_hots(i):
        info = meta[i].astype(F32)
        return info, [(place_iota == info[m : m + 1, :]) for m in range(MEMBERS)]

    def select(i):
        @pl.when(i > 0)
        def _():
            meta_copy(i).wait_recv()

        _, hots = one_hots(i)
        pick = jnp.concatenate([h.astype(F32) for h in hots], axis=0).astype(BF16)[:, :slots]
        for h in range(PARTS):
            @pl.when(i > 0)
            def _():
                s1_copy(i, h).wait_recv()

            for cols in chunks(part, 512):
                sel[i, h, :, :, cols] = split_rows(dot(pick, blk[i, h, :, cols]), MEMBERS)
            for k in (2, 3, 1):
                s2_copy(i, h, k).start()
            rows[i, h, member] = sel[i, h, member]

    def ffn(i, is_first):
        @pl.when(is_first)
        def _():
            for load in loads:
                load.wait()

        landed(rows.at[i, :, 1:], s2_recv.at[i])
        xs = [merge_rows(rows[i, h]) for h in range(PARTS)]
        for cols in chunks(ff, 256):
            gate_part = sum(dot(x, wg[h * part : (h + 1) * part, cols]) for h, x in enumerate(xs))
            up_part = sum(dot(x, wu[h * part : (h + 1) * part, cols]) for h, x in enumerate(xs))
            hidden[:, cols] = (gate_part / (1.0 + jnp.exp(-gate_part)) * up_part).astype(BF16)
        hid = hidden[...]
        for h in range(PARTS):
            for cols in chunks(part, 256):
                source = slice(h * part + cols.start, h * part + cols.stop)
                outs[i, h, :, :, cols] = split_rows(dot(hid, wd[:, source]), MEMBERS)
            for k in (2, 3, 1):
                r2_copy(i, h, k).start()
            obuf[i, h, member] = outs[i, h, member]

    def mix(i):
        info, hots = one_hots(i)

        def weights(row):
            parts = [jnp.where(hots[m], info[row + m : row + m + 1, :], 0.0) for m in range(MEMBERS)]
            return jnp.concatenate(parts, axis=0).T[:slots].astype(BF16)

        high, low = weights(8), weights(16)

        def mixed(h, cols):
            values = merge_rows(obuf[i, h, :, :, cols])
            return (dot(high, values) + dot(low, values)).astype(BF16)

        for h in range(PARTS):
            landed(obuf.at[i, h, 1:], r2_recv.at[i, h])

            @pl.when(i == 0)
            def _():
                for cols in chunks(part, 512):
                    back[0, h, :, cols] = mixed(h, cols)

            @pl.when(i > 0)
            def _():
                for cols in chunks(part, 512):
                    comb[i, h, :, cols] = mixed(h, cols)
                r1_copy(i, h).start()

    plans = [plan(groups, False), plan(groups, True)]
    length = max(len(p[0]) for p in plans)
    outer = (group // (groups // 2)) % 2 == (group // (groups // 4)) % 2

    def planned(kind, t):
        inner_table, outer_table = (p[kind] + [-1] * (length - len(p[kind])) for p in plans)
        return jnp.where(outer, entry(outer_table, t), entry(inner_table, t))

    first_outputs = [next(t for t, i in enumerate(p[2]) if i >= 0) for p in plans]
    first_output = jnp.where(outer, first_outputs[1], first_outputs[0])

    @pl.loop(0, length)
    def _(t):
        to_select, to_mix, to_output = planned(0, t), planned(1, t), planned(2, t)

        @pl.when(to_select >= 0)
        def _():
            select(to_select)

        for d in range(2, distances + 1):
            @pl.when(t == d - 2)
            def _():
                send(d)

        @pl.when(t == 1)
        def _():
            key_column = jnp.broadcast_to(key.astype(F32), (LANES, tok)).T[:, 0:1].astype(jnp.int32)
            spread_ref[...] = (
                lax.broadcasted_iota(jnp.int32, (tok, groups * slots), 1) == key_column
            ).astype(F32).astype(BF16)

        @pl.when(to_mix >= 0)
        def _():
            mix(to_mix)

        @pl.when(to_output >= 0)
        def _():
            ffn(to_output, t == first_output)

    landed(pack.at[1:], s1_send.at[0])
    landed(pack_meta.at[1:], m_send.at[0])
    landed(sel.at[:, :, 1:], s2_send.at[0])
    landed(outs.at[:, :, 1:], r2_send.at[0])
    landed(comb.at[1:], r1_send.at[0])
    landed(back.at[1:], r1_recv.at[0])
    for h in range(PARTS):
        for cols in chunks(part, 512):
            target = pl.ds(h * part + cols.start, cols.stop - cols.start)
            out_ref[:, target] = dot(spread_ref[...], merge_rows(back[:, h, :, cols])).astype(BF16)


def shards(tokens, norm_gain, expert_ids, gates, w_gate, w_up, w_down):
    tok, width = tokens.shape
    ff = w_gate.shape[2]
    experts = lax.axis_size("ep")
    groups = experts // MEMBERS
    cap = 2 * ((2 * tok + experts - 1) // experts)
    slots = 2 * cap
    hbm = pl.BlockSpec(memory_space=pltpu.HBM)
    dma = pltpu.SemaphoreType.DMA
    by_group = pltpu.VMEM((groups, PARTS, slots, width // PARTS), BF16)
    by_member = pltpu.VMEM((groups, PARTS, MEMBERS, cap, width // PARTS), BF16)
    facts = pltpu.VMEM((groups, 32, LANES), BF16)
    return pl.pallas_call(
        functools.partial(kernel, groups, cap),
        out_shape=jax.ShapeDtypeStruct((tok, width), BF16),
        in_specs=[hbm] * 7,
        out_specs=pl.BlockSpec(memory_space=pltpu.VMEM),
        scratch_shapes=[
            pltpu.VMEM((tok, groups * slots), BF16),
            pltpu.VMEM((2, tok), jnp.int32), pltpu.VMEM((2, tok), F32),
            pltpu.VMEM((tok, width), BF16), pltpu.VMEM((1, width), F32),
            pltpu.VMEM((width, ff), BF16), pltpu.VMEM((width, ff), BF16), pltpu.VMEM((ff, width), BF16),
            pltpu.VMEM((tok, width), BF16),
            by_group, facts, by_group, facts, by_member, by_member,
            pltpu.VMEM((MEMBERS * cap, ff), BF16),
            by_member, by_member, by_group, by_group,
            dma((3 + tok // min(tok, 64),)), dma((3,)), pltpu.SemaphoreType.REGULAR((groups.bit_length(),)),
            dma((1,)), dma((groups, PARTS)), dma((1,)), dma((groups,)),
            dma((1,)), dma((groups,)), dma((1,)), dma((groups, PARTS)), dma((1,)), dma((1,)),
        ],
        compiler_params=pltpu.CompilerParams(
            collective_id=0, has_side_effects=True, vmem_limit_bytes=50 * 1024 * 1024
        ),
    )(*[pltpu.with_memory_space_constraint(a, pltpu.HBM) for a in (expert_ids.T, gates.T, tokens, norm_gain.reshape(1, width), w_gate, w_up, w_down)])


def solution(mesh):
    return jax.shard_map(
        shards,
        mesh=mesh,
        in_specs=(
            P("ep", None),
            P(),
            P("ep", None),
            P("ep", None),
            P("ep", None, None),
            P("ep", None, None),
            P("ep", None, None),
        ),
        out_specs=P("ep", None),
        check_vma=False,
    )
```

```python
import functools

import jax
import jax.numpy as jnp
from jax import lax
from jax.experimental import pallas as pl
from jax.experimental.pallas import tpu as pltpu
from jax.sharding import PartitionSpec as P

EPS = 1e-06
MEMBERS = 4
LANES = 128
MESH = pl.DeviceIdType.MESH
F32 = jnp.float32
BF16 = jnp.bfloat16


def xor(a, b, count):
    total, bit = 0, 1
    while bit < count:
        total = total + ((a // bit + b // bit) % 2) * bit
        bit *= 2
    return total


def bits(i):
    return bin(i).count("1")


def halves(groups):
    half = groups // 2
    upper = sorted(range(half, groups), key=lambda i: (bits(i), -i))
    lower = sorted(range(1, half), key=lambda i: (bits(i), i))
    return upper, lower


def send_order(groups, distance):
    upper, lower = ([i for i in items if bits(i) == distance] for items in halves(groups))
    if distance == 1:
        return lower + upper
    order = []
    while upper or lower:
        order += upper[:1] + lower[:1]
        upper, lower = upper[1:], lower[1:]
    return order


def plan(groups, outer):
    upper, lower = halves(groups)
    near = [i for i in lower if bits(i) == 1]
    rest = [i for i in lower if bits(i) > 1]
    steps, waiting = [], []

    def select(*items):
        steps.extend((0, i) for i in items)

    def mix(keep):
        while len(waiting) > keep:
            steps.append((1, waiting.pop(0)))

    def output(*items):
        steps.extend((2, i) for i in items)
        waiting.extend(items)

    select(0, *near, upper[0])
    output(near[0])
    select(upper[1])
    output(upper[0])
    if outer:
        select(*rest)
    else:
        output(*near[1:])
    for before, i in zip(upper[1:], upper[2:]):
        select(i)
        mix(1)
        output(before)
    mix(1)
    if outer:
        output(upper[-1], *rest)
        mix(len(rest) + 1)
        output(*near[1:])
        mix(len(near))
        output(0)
    else:
        select(*rest)
        output(upper[-1])
        mix(1)
        output(*rest, 0)
    mix(0)

    rows, last = [], 2
    for kind, item in steps:
        if kind <= last:
            rows.append([-1, -1, -1])
        rows[-1][kind] = item
        last = kind
    return [list(column) for column in zip(*rows)]


PARTS = 2


def entry(table, t):
    return sum(jnp.where(t == k, value, 0) for k, value in enumerate(table) if value)


def merge_rows(block):
    parts, rows, width = block.shape
    if rows % 16 == 0:
        return block.reshape(parts * rows, width)
    return block.astype(F32).reshape(parts * rows, width).astype(BF16)


def split_rows(block, parts):
    rows, width = block.shape
    return block.reshape(parts, rows // parts, width).astype(BF16)


def chunks(width, size):
    size = min(width, size)
    return [slice(start, start + size) for start in range(0, width, size)]


def dot(a, b):
    return jnp.dot(a, b, preferred_element_type=F32)


def kernel(
    groups, cap,
    ids_hbm, gates_hbm, tokens_hbm, gain_hbm, wg_hbm, wu_hbm, wd_hbm, out_ref,
    spread_ref,
    ids_ref, gates_ref, tokens_ref, gain_ref, wg, wu, wd, normed, pack, pack_meta, blk, meta, sel, rows, hidden, outs, obuf, comb, back,
    in_sem, w_sem, near_sem, s1_send, s1_recv, m_send, m_recv, s2_send, s2_recv, r2_send, r2_recv, r1_send, r1_recv,
):
    tok, width = tokens_ref.shape
    ff = wg.shape[1]
    slots = 2 * cap
    experts = groups * MEMBERS
    me = lax.axis_index("ep")
    group, member = me // MEMBERS, me % MEMBERS

    def far(i):
        return xor(group, i, groups) * MEMBERS + member

    def near(k):
        return group * MEMBERS + xor(member, k, MEMBERS)

    distances = bits(groups - 1)
    barrier = pltpu.get_barrier_semaphore()
    for k in range(1, MEMBERS):
        pl.semaphore_signal(barrier, inc=1, device_id=(near(k),), device_id_type=MESH)
    for b in range(distances):
        pl.semaphore_signal(barrier, inc=1, device_id=(far(2**b),), device_id_type=MESH)

    block = min(tok, 64)
    small = [
        pltpu.make_async_copy(src, dst, in_sem.at[k])
        for k, (src, dst) in enumerate(((ids_hbm, ids_ref), (gates_hbm, gates_ref), (gain_hbm, gain_ref)))
    ]
    token_loads = [
        pltpu.make_async_copy(
            tokens_hbm.at[pl.ds(r, block)], tokens_ref.at[pl.ds(r, block)], in_sem.at[3 + r // block]
        )
        for r in range(0, tok, block)
    ]
    loads = [
        pltpu.make_async_copy(src.at[0], dst, w_sem.at[k])
        for k, (src, dst) in enumerate(((wg_hbm, wg), (wu_hbm, wu), (wd_hbm, wd)))
    ]
    for load in small + token_loads:
        load.start()
    for load in small:
        load.wait()

    ids = ids_ref[...]
    first, second = ids[0:1, :], ids[1:2, :]
    before = (
        lax.broadcasted_iota(jnp.int32, (tok, tok), 0) < lax.broadcasted_iota(jnp.int32, (tok, tok), 1)
    ).astype(F32).astype(BF16)
    expert_iota = lax.broadcasted_iota(jnp.int32, (experts, tok), 0)
    is_first = (expert_iota == first).astype(F32)
    is_second = (expert_iota == second).astype(F32)
    earlier = dot((is_first + is_second).astype(BF16), before)
    place_first = jnp.sum(earlier * is_first, axis=0, keepdims=True) + 1.0
    place_second = jnp.sum(earlier * is_second, axis=0, keepdims=True) + 1.0
    token_group = first // MEMBERS
    group_rows = max(groups, 8)
    is_group = (lax.broadcasted_iota(jnp.int32, (group_rows, tok), 0) == token_group).astype(F32)
    slot = jnp.sum(dot(is_group.astype(BF16), before) * is_group, axis=0, keepdims=True).astype(jnp.int32)
    step_of = xor(token_group, jnp.full_like(token_group, group), groups)
    key = step_of * slots + slot

    local_first, local_second = first % MEMBERS, second % MEMBERS
    gates = gates_ref[...]
    gate_high = gates.astype(BF16).astype(F32)
    gate_low = (gates - gate_high).astype(BF16).astype(F32)

    def member_rows(of_first, of_second):
        m = lax.broadcasted_iota(jnp.int32, (8, tok), 0)
        return jnp.where(m == local_first, of_first, 0.0) + jnp.where(m == local_second, of_second, 0.0)

    facts = jnp.concatenate(
        [
            member_rows(place_first, place_second),
            member_rows(gate_high[0:1, :], gate_high[1:2, :]),
            member_rows(gate_low[0:1, :], gate_low[1:2, :]),
            jnp.zeros((8, tok), F32),
        ],
        axis=0,
    ).astype(BF16)
    pick_iota = lax.broadcasted_iota(jnp.int32, (groups * slots, tok), 0)
    picked = (pick_iota == key).astype(F32).astype(BF16)
    wide_iota = lax.broadcasted_iota(jnp.int32, (groups * LANES, tok), 0)
    wide = (wide_iota == step_of * LANES + slot).astype(F32).astype(BF16)
    told = lax.dot_general(
        facts, wide, (((1,), (1,)), ((), ())), preferred_element_type=F32
    ).astype(BF16)
    meta[0] = told[:, :LANES]
    for i in range(1, groups):
        pack_meta[i] = told[:, i * LANES : (i + 1) * LANES]
    for r in range(0, tok, min(tok, 16)):
        if r % block == 0:
            token_loads[r // block].wait()
        lines = pl.ds(r, min(tok, 16))
        floats = tokens_ref[lines, :].astype(F32)
        inverse = lax.rsqrt(jnp.mean(floats * floats, axis=-1, keepdims=True) + EPS)
        normed[lines, :] = (floats * inverse * gain_ref[...]).astype(BF16)

    for load in loads:
        load.start()

    part = width // PARTS
    for h in range(PARTS):
        for cols in chunks(part, 256):
            source = slice(h * part + cols.start, h * part + cols.stop)
            packed = split_rows(dot(picked, normed[:, source]), groups)
            blk[0, h, :, cols] = packed[0]
            pack[1:, h, :, cols] = packed[1:]

    def s1_copy(i, h):
        return pltpu.make_async_remote_copy(
            src_ref=pack.at[i, h], dst_ref=blk.at[i, h], send_sem=s1_send.at[0], recv_sem=s1_recv.at[i, h],
            device_id=(far(i),), device_id_type=MESH,
        )

    def meta_copy(i):
        return pltpu.make_async_remote_copy(
            src_ref=pack_meta.at[i], dst_ref=meta.at[i], send_sem=m_send.at[0], recv_sem=m_recv.at[i],
            device_id=(far(i),), device_id_type=MESH,
        )

    def s2_copy(i, h, k):
        peer = xor(member, k, MEMBERS)
        return pltpu.make_async_remote_copy(
            src_ref=sel.at[i, h, peer], dst_ref=rows.at[i, h, member],
            send_sem=s2_send.at[0], recv_sem=s2_recv.at[i],
            device_id=(near(k),), device_id_type=MESH,
        )

    def r2_copy(i, h, k):
        peer = xor(member, k, MEMBERS)
        return pltpu.make_async_remote_copy(
            src_ref=outs.at[i, h, peer], dst_ref=obuf.at[i, h, member],
            send_sem=r2_send.at[0], recv_sem=r2_recv.at[i, h],
            device_id=(near(k),), device_id_type=MESH,
        )

    def r1_copy(i, h):
        return pltpu.make_async_remote_copy(
            src_ref=comb.at[i, h], dst_ref=back.at[i, h], send_sem=r1_send.at[0], recv_sem=r1_recv.at[0],
            device_id=(far(i),), device_id_type=MESH,
        )

    def landed(ref, sem):
        pltpu.make_async_copy(ref, ref, sem).wait()

    def send(distance):
        if distance == 1:
            pl.semaphore_wait(barrier, MEMBERS - 1 + distances)
        else:
            pl.semaphore_wait(near_sem.at[distance], distances)
        if distance < distances:
            for b in range(distances):
                pl.semaphore_signal(
                    near_sem.at[distance + 1], inc=1, device_id=(far(2**b),), device_id_type=MESH
                )
        for i in send_order(groups, distance):
            meta_copy(i).start()
            for h in range(PARTS):
                s1_copy(i, h).start()

    send(1)

    place_iota = lax.broadcasted_iota(jnp.int32, (cap, LANES), 0).astype(F32) + 1.0

    def one_hots(i):
        info = meta[i].astype(F32)
        return info, [(place_iota == info[m : m + 1, :]) for m in range(MEMBERS)]

    def select(i):
        @pl.when(i > 0)
        def _():
            meta_copy(i).wait_recv()

        _, hots = one_hots(i)
        pick = jnp.concatenate([h.astype(F32) for h in hots], axis=0).astype(BF16)[:, :slots]
        for h in range(PARTS):
            @pl.when(i > 0)
            def _():
                s1_copy(i, h).wait_recv()

            for cols in chunks(part, 512):
                sel[i, h, :, :, cols] = split_rows(dot(pick, blk[i, h, :, cols]), MEMBERS)
            for k in (2, 3, 1):
                s2_copy(i, h, k).start()
            rows[i, h, member] = sel[i, h, member]

    def ffn(i, is_first):
        @pl.when(is_first)
        def _():
            for load in loads:
                load.wait()

        landed(rows.at[i, :, 1:], s2_recv.at[i])
        xs = [merge_rows(rows[i, h]) for h in range(PARTS)]
        for cols in chunks(ff, 256):
            gate_part = sum(dot(x, wg[h * part : (h + 1) * part, cols]) for h, x in enumerate(xs))
            up_part = sum(dot(x, wu[h * part : (h + 1) * part, cols]) for h, x in enumerate(xs))
            hidden[:, cols] = (gate_part / (1.0 + jnp.exp(-gate_part)) * up_part).astype(BF16)
        hid = hidden[...]
        for h in range(PARTS):
            for cols in chunks(part, 256):
                source = slice(h * part + cols.start, h * part + cols.stop)
                outs[i, h, :, :, cols] = split_rows(dot(hid, wd[:, source]), MEMBERS)
            for k in (2, 3, 1):
                r2_copy(i, h, k).start()
            obuf[i, h, member] = outs[i, h, member]

    def mix(i):
        info, hots = one_hots(i)

        def weights(row):
            parts = [jnp.where(hots[m], info[row + m : row + m + 1, :], 0.0) for m in range(MEMBERS)]
            return jnp.concatenate(parts, axis=0).T[:slots].astype(BF16)

        high, low = weights(8), weights(16)

        def mixed(h, cols):
            values = merge_rows(obuf[i, h, :, :, cols])
            return (dot(high, values) + dot(low, values)).astype(BF16)

        for h in range(PARTS):
            landed(obuf.at[i, h, 1:], r2_recv.at[i, h])

            @pl.when(i == 0)
            def _():
                for cols in chunks(part, 512):
                    back[0, h, :, cols] = mixed(h, cols)

            @pl.when(i > 0)
            def _():
                for cols in chunks(part, 512):
                    comb[i, h, :, cols] = mixed(h, cols)
                r1_copy(i, h).start()

    plans = [plan(groups, False), plan(groups, True)]
    length = max(len(p[0]) for p in plans)
    outer = (group // (groups // 2)) % 2 == (group // (groups // 4)) % 2

    def planned(kind, t):
        inner_table, outer_table = (p[kind] + [-1] * (length - len(p[kind])) for p in plans)
        return jnp.where(outer, entry(outer_table, t), entry(inner_table, t))

    first_outputs = [next(t for t, i in enumerate(p[2]) if i >= 0) for p in plans]
    first_output = jnp.where(outer, first_outputs[1], first_outputs[0])

    @pl.loop(0, length)
    def _(t):
        to_select, to_mix, to_output = planned(0, t), planned(1, t), planned(2, t)

        @pl.when(to_select >= 0)
        def _():
            select(to_select)

        for d in range(2, distances + 1):
            @pl.when(t == d - 2)
            def _():
                send(d)

        @pl.when(t == 1)
        def _():
            key_column = jnp.broadcast_to(key.astype(F32), (LANES, tok)).T[:, 0:1].astype(jnp.int32)
            spread_ref[...] = (
                lax.broadcasted_iota(jnp.int32, (tok, groups * slots), 1) == key_column
            ).astype(F32).astype(BF16)

        @pl.when(to_mix >= 0)
        def _():
            mix(to_mix)

        @pl.when(to_output >= 0)
        def _():
            ffn(to_output, t == first_output)

    landed(pack.at[1:], s1_send.at[0])
    landed(pack_meta.at[1:], m_send.at[0])
    landed(sel.at[:, :, 1:], s2_send.at[0])
    landed(outs.at[:, :, 1:], r2_send.at[0])
    landed(comb.at[1:], r1_send.at[0])
    landed(back.at[1:], r1_recv.at[0])
    for h in range(PARTS):
        for cols in chunks(part, 256):
            target = pl.ds(h * part + cols.start, cols.stop - cols.start)
            out_ref[:, target] = dot(spread_ref[...], merge_rows(back[:, h, :, cols])).astype(BF16)


def shards(tokens, norm_gain, expert_ids, gates, w_gate, w_up, w_down):
    tok, width = tokens.shape
    ff = w_gate.shape[2]
    experts = lax.axis_size("ep")
    groups = experts // MEMBERS
    cap = 2 * ((2 * tok + experts - 1) // experts)
    slots = 2 * cap
    hbm = pl.BlockSpec(memory_space=pltpu.HBM)
    dma = pltpu.SemaphoreType.DMA
    by_group = pltpu.VMEM((groups, PARTS, slots, width // PARTS), BF16)
    by_member = pltpu.VMEM((groups, PARTS, MEMBERS, cap, width // PARTS), BF16)
    facts = pltpu.VMEM((groups, 32, LANES), BF16)
    return pl.pallas_call(
        functools.partial(kernel, groups, cap),
        out_shape=jax.ShapeDtypeStruct((tok, width), BF16),
        in_specs=[hbm] * 7,
        out_specs=pl.BlockSpec(memory_space=pltpu.VMEM),
        scratch_shapes=[
            pltpu.VMEM((tok, groups * slots), BF16),
            pltpu.VMEM((2, tok), jnp.int32), pltpu.VMEM((2, tok), F32),
            pltpu.VMEM((tok, width), BF16), pltpu.VMEM((1, width), F32),
            pltpu.VMEM((width, ff), BF16), pltpu.VMEM((width, ff), BF16), pltpu.VMEM((ff, width), BF16),
            pltpu.VMEM((tok, width), BF16),
            by_group, facts, by_group, facts, by_member, by_member,
            pltpu.VMEM((MEMBERS * cap, ff), BF16),
            by_member, by_member, by_group, by_group,
            dma((3 + tok // min(tok, 64),)), dma((3,)), pltpu.SemaphoreType.REGULAR((groups.bit_length(),)),
            dma((1,)), dma((groups, PARTS)), dma((1,)), dma((groups,)),
            dma((1,)), dma((groups,)), dma((1,)), dma((groups, PARTS)), dma((1,)), dma((1,)),
        ],
        compiler_params=pltpu.CompilerParams(
            collective_id=0, has_side_effects=True, vmem_limit_bytes=50 * 1024 * 1024
        ),
    )(*[pltpu.with_memory_space_constraint(a, pltpu.HBM) for a in (expert_ids.T, gates.T, tokens, norm_gain.reshape(1, width), w_gate, w_up, w_down)])


def solution(mesh):
    return jax.shard_map(
        shards,
        mesh=mesh,
        in_specs=(
            P("ep", None),
            P(),
            P("ep", None),
            P("ep", None),
            P("ep", None, None),
            P("ep", None, None),
            P("ep", None, None),
        ),
        out_specs=P("ep", None),
        check_vma=False,
    )
```
